32 devices in a mesh: grp: 2 (over y), tp: 4 (over z), dp: 4 (over x, core).
Axes of the slice: x: 2, y: 2, z: 4, core: 2. Of those that a mesh axis runs over, the one named last changes fastest.
Arguments:
- tokens: bfloat16 [512, 4096], P('grp', 'dp'), parts along dimension 0, may hold values from -40 to 40
- sequence_lengths: int32 [512], P(('grp', 'dp')), parts along dimension 0, may hold values from 1 to 4096, 262144 in all
- recurrent_state: float32 [2, 512, 128, 128], P(None, ('grp', 'dp'), 'tp'), parts along dimension 1, may hold values from -1.8 to 1.8
- norm_weight: float32 [2, 4096], P(None, 'dp'), may hold values from 0.1 to 1.9
- input_weight: bfloat16 [2, 4096, 2048], P(None, 'dp', 'tp'), may hold values from -0.09375 to 0.09375
- gate_weight: bfloat16 [2, 4096, 2048], P(None, 'dp', 'tp'), may hold values from -0.09375 to 0.09375
- output_weight: bfloat16 [2, 2048, 4096], P(None, 'tp', 'dp'), may hold values from -0.125 to 0.125
- negated_real_rate: float32 [2, 8192], P(None, 'tp'), may hold values from 0.005 to 1
- frequency: float32 [2, 8192], P(None, 'tp'), may hold values from -4 to 4
- discrete_step: float32 [2, 128], P(None, 'tp'), may hold values from 0.02 to 0.5
- group_input_matrix: float32 [2, 128, 16, 128], P(None, 'tp'), may hold values from -1.5 to 1.5
- group_output_matrix: float32 [2, 128, 16, 128], P(None, 'tp'), may hold values from -0.5 to 0.5
- feedthrough_weight: float32 [2, 2048], P(None, 'tp'), may hold values from -3 to 3
- extra_log_decay: float32 [2, 128, 4096], P(None, 'tp'), may hold values from -0.7 to 0
Outputs:
- tokens_out: bfloat16 [512, 4096], P('grp', 'dp'), parts along dimension 0
- state_out: float32 [2, 512, 128, 128], P(None, ('grp', 'dp'), 'tp'), parts along dimension 1
The draws below stay inside these ranges and needn't reach their ends.
There are 2 independent parts, one for each index of `grp`. The reference program is written for one: setup_inputs(seed, part) draws one part's arguments, and reference() takes and returns one part's arrays. A program takes and returns all parts, laid end to end along the dimension named above; an argument that names none is the same for every part. Nothing has to cross between parts.
Inputs may be any that keep to these rules, and one draw needn't show every extreme that they name: The newest token of a sequence stands at position sequence_lengths - 1.
All inputs are finite; a program needn't handle non-finite values. No bound on the sum of `sequence_lengths` on one device may be relied on, other than what follows from the above.
Results may differ from the reference program's by a relative error of at most 0.009.
Values may be sent and summed in bfloat16 or wider, within the bound.
A program may use at most 64 MiB of HBM per device.

```python
import math
import jax
import jax.numpy as jnp
import numpy as np
from jax import lax

D = 4096
N = 2048
GROUP = 16
P_SIZE = 64
CHANNEL_GROUPS = 128
STACKED_LAYERS = 2
BATCH = 256
LONGEST_LENGTH = 4096
MEAN_LEN = 1024


def draw_tokens(key, part):
    key_base = jax.random.fold_in(key, 11)
    key_rows = jax.random.fold_in(key, 12)
    key_cols = jax.random.fold_in(key, 13)
    base = jnp.clip(jax.random.normal(key_base, (BATCH, D), jnp.float32), -4.0, 4.0)
    rising = 4.0
    row_scale = jnp.exp(jax.random.uniform(key_rows, (BATCH, 1), jnp.float32, math.log(0.3), math.log(3.0)))
    column_pos = jnp.arange(D, dtype=jnp.float32)[None, :] / D
    jitter = jnp.exp(jax.random.uniform(key_cols, (1, D), jnp.float32, -0.5, 0.5))
    col_scale = 0.5 * jnp.exp(math.log(rising) * column_pos) * jitter
    return (base * row_scale * col_scale).astype(jnp.bfloat16)


def level_of(key, dims, pieces, least, largest):
    def one(position, blocks):
        heights = jax.random.uniform(jax.random.fold_in(jax.random.fold_in(key, 6), position), (blocks,), jnp.float32, least / len(pieces), largest / len(pieces))
        return jnp.repeat(jnp.exp(heights), dims[position] // blocks).reshape((-1,) + (1,) * (len(dims) - position - 1))

    loudness = one(*pieces[0])
    for cut in pieces[1:]:
        loudness = loudness * one(*cut)
    return loudness


def profile(amount, total, most, slope):
    weights = [(1 << 20) // math.isqrt(grade ** slope) + 1 for grade in range(2, amount + 1)]
    rest, counts = total - most - (amount - 1), [1] * (amount - 1)
    while rest > 0:
        free = [i for i in range(amount - 1) if counts[i] < most]
        mass, left = sum([weights[i] for i in free]), rest
        for i in free:
            addition = min(most - counts[i], max(1, left * weights[i] // mass), rest)
            counts[i] = counts[i] + addition
            rest = rest - addition
    return np.array([most] + counts)


def uneven_parts(stream_key, amount, total, bound, skew):
    if amount == 2:
        one = jax.random.randint(stream_key, (), max(1, total - bound), min(bound, total - 1) + 1)
        return jnp.stack([one, total - one])
    lengths = jnp.asarray(profile(amount, total, bound, skew), jnp.int32)
    couples = (amount - 1) // 2
    source_of, receiver = lengths[1:1 + 2 * couples:2], lengths[2:2 + 2 * couples:2]
    margin = jnp.minimum(source_of - 1, bound - receiver)
    passed = jax.random.randint(jax.random.fold_in(stream_key, 1), (couples,), 0, 1 << 20) % (margin + 1)
    lengths = lengths.at[1:1 + 2 * couples:2].set(source_of - passed).at[2:2 + 2 * couples:2].set(receiver + passed)
    return lengths[jax.random.permutation(jax.random.fold_in(stream_key, 2), amount)]


def centred(key, dims, scale, limit, split=(), kind=jnp.bfloat16):
    gain = level_of(key, dims, split, -0.22, 0.18) if split else 1.0
    values = jax.random.normal(key, dims, jnp.float32) * scale * gain
    return jnp.minimum(jnp.maximum(values, -limit), limit).astype(kind)


def setup_inputs(seed: int = 0, part: int = 0) -> dict:
    arg_keys = jax.random.split(jax.random.key(seed), 15)
    own_keys = jax.random.split(jax.random.fold_in(arg_keys[14], part), 15)
    tokens = draw_tokens(jax.random.fold_in(jax.random.fold_in(arg_keys[14], part), 71), part)
    sequence_lengths = uneven_parts(own_keys[1], BATCH, BATCH * MEAN_LEN, LONGEST_LENGTH, 2).astype(jnp.int32)
    recurrent_state = centred(own_keys[2], (STACKED_LAYERS, BATCH, CHANNEL_GROUPS, 2 * P_SIZE), 0.3, 1.8, ((1, 4), (2, 4)), jnp.float32)
    norm_weight = jnp.clip(1.0 + 0.18 * jax.random.normal(arg_keys[3], (STACKED_LAYERS, D), jnp.float32), 0.1, 1.9)
    input_weight = centred(arg_keys[4], (STACKED_LAYERS, D, N), D ** -0.5, 0.09375, ((1, 4), (2, 4)))
    gate_weight = centred(arg_keys[5], (STACKED_LAYERS, D, N), D ** -0.5, 0.09375, ((1, 4), (2, 4)))
    output_weight = centred(arg_keys[6], (STACKED_LAYERS, N, D), N ** -0.5, 0.125, ((1, 4), (2, 4)))
    negated_real_rate = jnp.clip(jnp.exp(math.log(1.0) - 5.2983174 * jax.random.uniform(arg_keys[7], (STACKED_LAYERS, CHANNEL_GROUPS * P_SIZE), jnp.float32) ** level_of(arg_keys[7], (STACKED_LAYERS, CHANNEL_GROUPS * P_SIZE), ((1, 4),), -0.2, 0.2)), 0.005, 1.0)
    frequency = jnp.clip(jax.random.uniform(arg_keys[8], (STACKED_LAYERS, CHANNEL_GROUPS * P_SIZE), jnp.float32, -4.0, 4.0) * level_of(arg_keys[8], (STACKED_LAYERS, CHANNEL_GROUPS * P_SIZE), ((1, 4),), -0.4, 0.0), -4.0, 4.0)
    discrete_step = jnp.clip(jnp.exp(math.log(0.5) - 3.218876 * jax.random.uniform(arg_keys[9], (STACKED_LAYERS, CHANNEL_GROUPS), jnp.float32) ** level_of(arg_keys[9], (STACKED_LAYERS, CHANNEL_GROUPS), ((1, 4),), -0.2, 0.2)), 0.02, 0.5)
    group_input_matrix = centred(arg_keys[10], (STACKED_LAYERS, CHANNEL_GROUPS, GROUP, 2 * P_SIZE), GROUP ** -0.5, 1.5, ((1, 4),), jnp.float32)
    group_output_matrix = centred(arg_keys[11], (STACKED_LAYERS, CHANNEL_GROUPS, GROUP, 2 * P_SIZE), (2 * P_SIZE) ** -0.5, 0.5, ((1, 4),), jnp.float32)
    feedthrough_weight = centred(arg_keys[12], (STACKED_LAYERS, N), 0.5, 3.0, ((1, 4),), jnp.float32)
    extra_log_decay = jnp.clip(-0.7 + 0.7 * jax.random.uniform(arg_keys[13], (STACKED_LAYERS, CHANNEL_GROUPS, LONGEST_LENGTH), jnp.float32) ** level_of(arg_keys[13], (STACKED_LAYERS, CHANNEL_GROUPS, LONGEST_LENGTH), ((1, 4),), -0.2, 0.2), -0.7, 0.0)
    return dict(tokens=tokens, sequence_lengths=sequence_lengths, recurrent_state=recurrent_state, norm_weight=norm_weight, input_weight=input_weight, gate_weight=gate_weight, output_weight=output_weight, negated_real_rate=negated_real_rate, frequency=frequency, discrete_step=discrete_step, group_input_matrix=group_input_matrix, group_output_matrix=group_output_matrix, feedthrough_weight=feedthrough_weight, extra_log_decay=extra_log_decay)


TOP_PRECISION = lax.Precision.HIGHEST
NORM_EPS = 1e-06

def transition(decay_factor, angular_frequency, step_width):
    log_mag = -decay_factor * step_width[:, None]
    turn = angular_frequency * step_width[:, None]
    magnitude = jnp.exp(log_mag)
    discrete_real = magnitude * jnp.cos(turn)
    discrete_imaginary = magnitude * jnp.sin(turn)
    half_sine = jnp.sin(0.5 * turn)
    numer_re = jnp.expm1(log_mag) * jnp.cos(turn) - 2.0 * half_sine * half_sine
    numer_im = discrete_imaginary
    denom = decay_factor * decay_factor + angular_frequency * angular_frequency
    drive_re = (-numer_re * decay_factor + numer_im * angular_frequency) / denom
    drive_im = (-numer_im * decay_factor - numer_re * angular_frequency) / denom
    return (discrete_real, discrete_imaginary, drive_re, drive_im)

def state_space_update(input_groups, layer_state, extra_decay_factor, decay_factor, angular_frequency, step_width, input_matrix, readout_matrix):
    half_width = input_matrix.shape[-1] // 2
    decay_factor = decay_factor.reshape(-1, half_width)
    angular_frequency = angular_frequency.reshape(-1, half_width)
    discrete_real, discrete_imaginary, drive_re, drive_im = transition(decay_factor, angular_frequency, step_width)
    input_real = input_matrix[..., :half_width]
    input_imaginary = input_matrix[..., half_width:]
    driven_input_real = jnp.einsum('tkl,klf->tkf', input_groups, input_real, precision=TOP_PRECISION)
    driven_input_imaginary = jnp.einsum('tkl,klf->tkf', input_groups, input_imaginary, precision=TOP_PRECISION)
    state_re = layer_state[..., :half_width]
    state_im = layer_state[..., half_width:]
    carried_real = extra_decay_factor[..., None] * discrete_real[None]
    carried_imaginary = extra_decay_factor[..., None] * discrete_imaginary[None]
    updated_real = carried_real * state_re - carried_imaginary * state_im + drive_re[None] * driven_input_real - drive_im[None] * driven_input_imaginary
    updated_imaginary = carried_real * state_im + carried_imaginary * state_re + drive_re[None] * driven_input_imaginary + drive_im[None] * driven_input_real
    readout_rows = jnp.einsum('hzk,dhk->dhz', readout_matrix[..., :half_width], updated_real, precision=TOP_PRECISION) - jnp.einsum('hzk,dhk->dhz', readout_matrix[..., half_width:], updated_imaginary, precision=TOP_PRECISION)
    return (readout_rows, jnp.concatenate([updated_real, updated_imaginary], axis=-1))

def single_layer(hidden_rows, sequence_lengths, layer_state, norm_scale_rows, input_matrix_weight, gate_matrix, output_matrix_weight, decay_factor, angular_frequency, step_width, input_matrix, readout_matrix, feedthrough_rows, extra_decay_rows):
    x_float = hidden_rows.astype(jnp.float32)
    scale = lax.rsqrt(lax.optimization_barrier(jnp.mean(x_float * x_float, axis=1)) + NORM_EPS)[:, None]
    scaled_in = (x_float * norm_scale_rows[None, :]).astype(jnp.bfloat16)
    u_vals = (jnp.dot(scaled_in, input_matrix_weight, preferred_element_type=jnp.float32) * scale).astype(jnp.bfloat16)
    gate_vals = (jnp.dot(scaled_in, gate_matrix, preferred_element_type=jnp.float32) * scale).astype(jnp.bfloat16)
    batch_rows = hidden_rows.shape[0]
    group_count = layer_state.shape[1]
    input_float = u_vals.astype(jnp.float32)
    token_positions = (sequence_lengths - 1).astype(jnp.int32)
    extra_decay_factor = jnp.exp(jnp.take(extra_decay_rows, token_positions, axis=1).T)
    readout_rows, updated_state = state_space_update(input_float.reshape(batch_rows, group_count, -1), layer_state, extra_decay_factor, decay_factor, angular_frequency, step_width, input_matrix, readout_matrix)
    y_vals = jax.nn.gelu(readout_rows.reshape(batch_rows, -1) + feedthrough_rows[None, :] * input_float)
    mixed = (y_vals * jax.nn.sigmoid(gate_vals.astype(jnp.float32))).astype(jnp.bfloat16)
    branch = jnp.dot(mixed, output_matrix_weight, preferred_element_type=jnp.float32).astype(jnp.bfloat16)
    x_next = (x_float + branch.astype(jnp.float32)).astype(jnp.bfloat16)
    return (x_next, updated_state)

def reference(tokens, sequence_lengths, recurrent_state, norm_weight, input_weight, gate_weight, output_weight, negated_real_rate, frequency, discrete_step, group_input_matrix, group_output_matrix, feedthrough_weight, extra_log_decay):
    hidden_rows = tokens
    states = []
    for index_of_layer in range(STACKED_LAYERS):
        hidden_rows, updated_state = single_layer(hidden_rows, sequence_lengths, recurrent_state[index_of_layer], norm_weight[index_of_layer], input_weight[index_of_layer], gate_weight[index_of_layer], output_weight[index_of_layer], negated_real_rate[index_of_layer], frequency[index_of_layer], discrete_step[index_of_layer], group_input_matrix[index_of_layer], group_output_matrix[index_of_layer], feedthrough_weight[index_of_layer], extra_log_decay[index_of_layer])
        states.append(updated_state)
    return (hidden_rows, jnp.stack(states, axis=0))
```

```python
import functools

import jax
import jax.numpy as jnp
from jax import lax
from jax.experimental import pallas as pl
from jax.experimental.pallas import tpu as pltpu
from jax.sharding import PartitionSpec as P

NORM_EPS = 1e-06
MESH = pl.DeviceIdType.MESH
F32 = jnp.float32
BF16 = jnp.bfloat16
CHUNK_ROWS = 16
GELU_SLOPE = 0.7978845608028654

STAGE_AT = (0.0, 4.0, 8.0, 11.0, 16.0)
LAYER_AT = 20.0
CHUNK_AT = 3.0


def dot(a, b, contract=((1,), (0,)), precision=None):
    return lax.dot_general(
        a, b, (contract, ((), ())), preferred_element_type=F32, precision=precision
    )


def iota(shape, axis):
    return lax.broadcasted_iota(jnp.int32, shape, axis)


def expm1(x):
    p = jnp.full_like(x, 1.0 / 39916800.0)
    for d in (3628800.0, 362880.0, 40320.0, 5040.0, 720.0, 120.0, 24.0, 6.0, 2.0, 1.0):
        p = p * x + 1.0 / d
    return p * x


def column_of(row):
    n = row.shape[1]
    eye = iota((n, n), 0) == iota((n, n), 1)
    return jnp.sum(jnp.where(eye, row, 0.0), axis=1, keepdims=True)


def kernel(
    sizes,
    tok_ref,
    len_ref,
    state_ref,
    norm_ref,
    win_ref,
    wgate_ref,
    wout_ref,
    rate_ref,
    freq_ref,
    step_ref,
    gin_ref,
    gout_ref,
    feed_ref,
    decay_ref,
    out_tok,
    out_state,
    xs,
    st,
    norm,
    win,
    wgate,
    wout,
    rate,
    freq,
    step,
    gin,
    gout,
    feed,
    decay,
    kb,
    rb,
    pay,
    got,
    zb,
    part,
    own,
    ab,
    load_sem,
    rs_send,
    rs_recv,
    ag_send,
    ag_recv,
    ar_send,
    ar_recv,
    x_send,
    x_recv,
    out_sem,
):
    layers, dp, tp, chunks, rows, features = sizes
    groups, width = st.shape[2], st.shape[3]
    half = width // 2
    channels = win.shape[2]
    per_group = channels // groups
    blocks = groups // 8
    span = 8 * per_group
    total = features * dp
    pad = pay.shape[-1] - 2 * channels
    me = lax.axis_index("dp")
    z = lax.axis_index("tp")
    mid = tp // 2
    left = z < mid
    is_mid = jnp.logical_or(z == mid - 1, z == mid)
    is_end = jnp.logical_or(z == 0, z == tp - 1)
    inner = jnp.where(left, z + 1, z - 1)
    outer = jnp.where(left, z - 1, z + 1)
    peers = [lax.rem(me + k, dp) for k in range(1, dp)]

    loads = {}

    def load(name, src, dst):
        c = pltpu.make_async_copy(src, dst, load_sem.at[len(loads)])
        c.start()
        loads[name] = c

    load("x0", tok_ref.at[:, 0], xs.at[0, 0])
    load("norm", norm_ref, norm)
    load("win0", win_ref.at[0], win.at[0])
    load("wgate0", wgate_ref.at[0], wgate.at[0])
    for j in range(1, chunks):
        load(f"x{j}", tok_ref.at[:, j], xs.at[0, j])
    load("rate", rate_ref, rate)
    load("freq", freq_ref, freq)
    load("step", step_ref, step)
    load("decay", decay_ref, decay)
    load("gin", gin_ref, gin)
    load("gout", gout_ref, gout)
    load("feed", feed_ref, feed)
    load("state0", state_ref.at[0], st.at[0])
    load("wout0", wout_ref.at[0], wout.at[0])
    for l in range(1, layers):
        load(f"state{l}", state_ref.at[l], st.at[l])
        load(f"win{l}", win_ref.at[l], win.at[l])
        load(f"wgate{l}", wgate_ref.at[l], wgate.at[l])
        load(f"wout{l}", wout_ref.at[l], wout.at[l])
    waited = set()

    def need(*names):
        for name in names:
            if name not in waited:
                waited.add(name)
                loads[name].wait()

    barrier = pltpu.get_barrier_semaphore()
    for p in peers:
        pl.semaphore_signal(barrier, inc=1, device_id={"dp": p}, device_id_type=MESH)
    pl.semaphore_signal(barrier, inc=1, device_id={"tp": inner}, device_id_type=MESH)

    @pl.when(jnp.logical_not(is_end))
    def _():
        pl.semaphore_signal(barrier, inc=1, device_id={"tp": outer}, device_id_type=MESH)

    pl.semaphore_wait(barrier, dp - 1 + jnp.where(is_end, 1, 2))

    def remote(src, dst, send, recv, axis, peer):
        return pltpu.make_async_remote_copy(
            src_ref=src,
            dst_ref=dst,
            send_sem=send,
            recv_sem=recv,
            device_id={axis: peer},
            device_id_type=MESH,
        )

    def rs_copy(l, j, k):
        return remote(
            pay.at[l, j, peers[k]], got.at[l, j, k], rs_send.at[l, j, k], rs_recv.at[l, j, k], "dp", peers[k]
        )

    def ag_copy(l, j, k):
        return remote(
            zb.at[l, j, me], zb.at[l, j, me], ag_send.at[l, j, k], ag_recv.at[l, j, k], "dp", peers[k]
        )

    def ag_arrival(l, j, k):
        origin = lax.rem(me + dp - (k + 1), dp)
        return remote(
            zb.at[l, j, me], zb.at[l, j, origin], ag_send.at[l, j, k], ag_recv.at[l, j, k], "dp", peers[k]
        )

    def sum_copy(l, j):
        slot = jnp.where(is_mid, 1, 0)
        return remote(own.at[l, j], ab.at[l, j, slot], ar_send.at[l, j], ar_recv.at[l, j, slot], "tp", inner)

    def sum_arrival(l, j, slot):
        return remote(own.at[l, j], ab.at[l, j, slot], ar_send.at[l, j], ar_recv.at[l, j, slot], "tp", inner)

    def x_copy(l, j):
        return remote(xs.at[l + 1, j], xs.at[l + 1, j], x_send.at[l, j], x_recv.at[l, j], "tp", outer)

    def state_copy(l, j):
        r = pl.ds(j * rows, rows)
        return pltpu.make_async_copy(st.at[l, r], out_state.at[l, r], out_sem.at[0, l, j])

    def token_copy(j):
        return pltpu.make_async_copy(xs.at[layers, j], out_tok.at[:, j], out_sem.at[1, 0, j])

    mask = (iota((1, 8, span), 2) // per_group) == iota((1, 8, span), 1)

    def prepare_tables():
        need("rate", "freq", "step", "gin", "gout")
        wide = groups * half
        pick = (iota((groups, wide), 1) // half) == iota((groups, wide), 0)
        sel = ((iota((wide, width), 0) % half) == (iota((wide, width), 1) % half)).astype(F32)
        sign = jnp.where(iota((1, width), 1) < half, 1.0, -1.0)
        tables = []
        for l in range(layers):
            both = jnp.concatenate(
                [jnp.where(pick, rate[l : l + 1], 0.0), jnp.where(pick, freq[l : l + 1], 0.0)], axis=0
            )
            flat = dot(both, sel, precision=lax.Precision.HIGHEST)
            a, w = flat[:groups], flat[groups:]
            dt = column_of(step[l : l + 1])
            log_mag = -a * dt
            turn = w * dt
            magnitude = jnp.exp(log_mag)
            cosine = jnp.cos(turn)
            dre = magnitude * cosine
            dim = magnitude * jnp.sin(turn)
            hs = jnp.sin(0.5 * turn)
            nre = expm1(log_mag) * cosine - 2.0 * hs * hs
            den = a * a + w * w
            kre = (-nre * a + dim * w) / den
            kim = (-dim * a - nre * w) / den
            b = gin[l]
            rolled = pltpu.roll(b.reshape(groups * per_group, width), half, 1).reshape(b.shape)
            kb[l] = (kre[:, None, :] * b - (sign * kim)[:, None, :] * rolled).astype(BF16).reshape(
                groups * per_group, width
            )
            rb[l] = (gout[l] * sign[None]).astype(BF16).reshape(groups * per_group, width)
            tables.append((dre, -sign * dim))
        return tables

    def prepare_state(l, tables, position):
        need(f"state{l}", "decay")
        dre, dim = tables[l]
        lg = decay[l]
        hi = lg.astype(BF16)
        lo = (lg - hi.astype(F32)).astype(BF16)
        e = jnp.exp(dot(position, hi, ((1,), (1,))) + dot(position, lo, ((1,), (1,))))
        seqs = e.shape[0]
        spread = jnp.broadcast_to(e[:, None, :], (seqs, 8, groups))
        for b in range(blocks):
            here = iota((1, 8, groups), 2) == (iota((1, 8, groups), 1) + 8 * b)
            factor = jnp.sum(jnp.where(here, spread, 0.0), axis=-1, keepdims=True)
            g = slice(8 * b, 8 * b + 8)
            s = st[l, :, g, :]
            turned = pltpu.roll(s.reshape(seqs * 8, width), half, 1).reshape(s.shape)
            st[l, :, g, :] = factor * (dre[g][None] * s + dim[g][None] * turned)

    def project(l, j):
        if l == 0:
            need(f"x{j}", "norm")
        need(f"win{l}", f"wgate{l}")
        x = xs[l, j].reshape(dp * rows, features).astype(F32)
        squares = jnp.sum(x * x, axis=1, keepdims=True)
        xg = (x * norm[l : l + 1]).astype(BF16)
        pay[l, j, :, :, :channels] = dot(xg, win[l]).astype(BF16).reshape(dp, rows, channels)
        pay[l, j, :, :, channels : 2 * channels] = dot(xg, wgate[l]).astype(BF16).reshape(dp, rows, channels)
        hi = squares.astype(BF16).astype(F32)
        lane = iota((dp * rows, pad), 1) < pad // 2
        pay[l, j, :, :, 2 * channels :] = (
            jnp.where(lane, hi, squares - hi).astype(BF16).reshape(dp, rows, pad)
        )
        for k in range(dp - 1):
            rs_copy(l, j, k).start()

    def update(l, j):
        for k in range(dp - 1):
            rs_copy(l, j, k).wait_recv()
        acc = pay[l, j, me].astype(F32)
        for k in range(dp - 1):
            acc = acc + got[l, j, k].astype(F32)
        squares = jnp.sum(acc[:, 2 * channels :], axis=1, keepdims=True) * (2.0 / pad)
        scale = lax.rsqrt(squares / total + NORM_EPS)
        u = (acc[:, :channels] * scale).astype(BF16).astype(F32)
        gate = (acc[:, channels : 2 * channels] * scale).astype(BF16).astype(F32)
        r = slice(j * rows, (j + 1) * rows)
        reads = []
        for b in range(blocks):
            ub = u[:, b * span : (b + 1) * span]
            spread = jnp.where(mask, jnp.broadcast_to(ub[:, None, :], (rows, 8, span)), 0.0)
            drive = dot(spread.reshape(rows * 8, span).astype(BF16), kb[l, b * span : (b + 1) * span])
            g = slice(8 * b, 8 * b + 8)
            new = st[l, r, g, :] + drive.reshape(rows, 8, width)
            st[l, r, g, :] = new
            read = dot(
                new.reshape(rows * 8, width).astype(BF16), rb[l, b * span : (b + 1) * span], ((1,), (1,))
            )
            reads.append(jnp.sum(jnp.where(mask, read.reshape(rows, 8, span), 0.0), axis=1))
        state_copy(l, j).start()
        v = (jnp.concatenate(reads, axis=1) if blocks > 1 else reads[0]) + feed[l : l + 1] * u
        y = 0.5 * v * (1.0 + jnp.tanh(GELU_SLOPE * (v + 0.044715 * (v * v * v))))
        zb[l, j, me] = (y / (1.0 + jnp.exp(-gate))).astype(BF16)
        for k in range(dp - 1):
            ag_copy(l, j, k).start()

    def branch(l, j):
        need(f"wout{l}")
        for k in range(dp - 1):
            ag_arrival(l, j, k).wait_recv()
        term = dot(zb[l, j].reshape(dp * rows, channels), wout[l]).reshape(dp, rows, features)

        @pl.when(is_end)
        def _():
            own[l, j] = term.astype(BF16)
            sum_copy(l, j).start()

        @pl.when(jnp.logical_not(is_end))
        def _():
            part[l, j] = term

    def gather_in(l, j):
        @pl.when(jnp.logical_not(is_end))
        def _():
            sum_arrival(l, j, 0).wait_recv()
            own[l, j] = (part[l, j] + ab[l, j, 0].astype(F32)).astype(BF16)
            sum_copy(l, j).start()

    def finish(l, j):
        @pl.when(is_mid)
        def _():
            sum_arrival(l, j, 1).wait_recv()
            both = (own[l, j].astype(F32) + ab[l, j, 1].astype(F32)).astype(BF16)
            xs[l + 1, j] = (xs[l, j].astype(F32) + both.astype(F32)).astype(BF16)

        @pl.when(jnp.logical_not(is_mid))
        def _():
            x_copy(l, j).wait_recv()

        @pl.when(jnp.logical_not(is_end))
        def _():
            x_copy(l, j).start()

        if l == layers - 1:
            token_copy(j).start()

    stages = (project, update, branch, gather_in, finish)
    order = sorted(
        (l * LAYER_AT + STAGE_AT[s] + j * CHUNK_AT, l, s, j)
        for l in range(layers)
        for s in range(len(stages))
        for j in range(chunks)
    )
    tables = None
    prepared = set()
    for at, l, s, j in order:
        if s == 1 and tables is None:
            tables = prepare_tables()
            lengths = len_ref[...]
            places = decay.shape[2]
            position = (iota((lengths.shape[0], places), 1) == lengths - 1).astype(F32).astype(BF16)
            need("feed")
        if s == 1 and not prepared:
            for m in range(layers):
                prepared.add(m)
                prepare_state(m, tables, position)
        stages[s](l, j)

    for l in range(layers):
        for j in range(chunks):
            for k in range(dp - 1):
                rs_copy(l, j, k).wait_send()
                ag_copy(l, j, k).wait_send()
            sum_copy(l, j).wait_send()

            @pl.when(jnp.logical_not(is_end))
            def _():
                x_copy(l, j).wait_send()

            state_copy(l, j).wait()
    for j in range(chunks):
        token_copy(j).wait()


def on_device(
    dp,
    tp,
    tokens,
    sequence_lengths,
    recurrent_state,
    norm_weight,
    input_weight,
    gate_weight,
    output_weight,
    negated_real_rate,
    frequency,
    discrete_step,
    group_input_matrix,
    group_output_matrix,
    feedthrough_weight,
    extra_log_decay,
):
    batch, features = tokens.shape
    mine = sequence_lengths.shape[0]
    rows = CHUNK_ROWS if mine % CHUNK_ROWS == 0 else mine
    chunks = mine // rows
    layers = input_weight.shape[0]
    channels = input_weight.shape[2]
    pad = 128
    tall = 2 * channels + pad
    dma = pltpu.SemaphoreType.DMA
    any_spec = pl.BlockSpec(memory_space=pl.ANY)
    vmem = lambda a: pltpu.VMEM(a.shape, a.dtype)
    piece = (layers, chunks, dp, rows, features)
    n_tab = group_input_matrix.shape[1] * group_input_matrix.shape[2]
    width = group_input_matrix.shape[3]
    tok, state = pl.pallas_call(
        functools.partial(kernel, (layers, dp, tp, chunks, rows, features)),
        out_shape=(
            jax.ShapeDtypeStruct((dp, chunks, rows, features), BF16),
            jax.ShapeDtypeStruct(recurrent_state.shape, F32),
        ),
        in_specs=[any_spec, pl.BlockSpec(memory_space=pltpu.VMEM)] + [any_spec] * 12,
        out_specs=(any_spec, any_spec),
        scratch_shapes=[
            pltpu.VMEM((layers + 1,) + piece[1:], BF16),
            vmem(recurrent_state),
            vmem(norm_weight),
            vmem(input_weight),
            vmem(gate_weight),
            vmem(output_weight),
            vmem(negated_real_rate),
            vmem(frequency),
            vmem(discrete_step),
            vmem(group_input_matrix),
            vmem(group_output_matrix),
            vmem(feedthrough_weight),
            vmem(extra_log_decay),
            pltpu.VMEM((layers, n_tab, width), BF16),
            pltpu.VMEM((layers, n_tab, width), BF16),
            pltpu.VMEM((layers, chunks, dp, rows, tall), BF16),
            pltpu.VMEM((layers, chunks, dp - 1, rows, tall), BF16),
            pltpu.VMEM((layers, chunks, dp, rows, channels), BF16),
            pltpu.VMEM(piece, F32),
            pltpu.VMEM(piece, BF16),
            pltpu.VMEM((layers, chunks, 2, dp, rows, features), BF16),
            dma((9 + chunks + 4 * layers,)),
            dma((layers, chunks, dp - 1)),
            dma((layers, chunks, dp - 1)),
            dma((layers, chunks, dp - 1)),
            dma((layers, chunks, dp - 1)),
            dma((layers, chunks)),
            dma((layers, chunks, 2)),
            dma((layers, chunks)),
            dma((layers, chunks)),
            dma((2, layers, chunks)),
        ],
        compiler_params=pltpu.CompilerParams(
            collective_id=0, has_side_effects=True, vmem_limit_bytes=60 * 1024 * 1024
        ),
    )(
        tokens.reshape(dp, chunks, rows, features),
        sequence_lengths.reshape(mine, 1),
        recurrent_state,
        norm_weight,
        input_weight,
        gate_weight,
        output_weight,
        negated_real_rate,
        frequency,
        discrete_step,
        group_input_matrix,
        group_output_matrix,
        feedthrough_weight,
        extra_log_decay,
    )
    return tok.reshape(batch, features), state


def solution(mesh):
    in_specs = (
        P("grp", "dp"),
        P(("grp", "dp")),
        P(None, ("grp", "dp"), "tp", None),
        P(None, "dp"),
        P(None, "dp", "tp"),
        P(None, "dp", "tp"),
        P(None, "tp", "dp"),
        P(None, "tp"),
        P(None, "tp"),
        P(None, "tp"),
        P(None, "tp", None, None),
        P(None, "tp", None, None),
        P(None, "tp"),
        P(None, "tp", None),
    )
    out_specs = (P("grp", "dp"), P(None, ("grp", "dp"), "tp", None))
    return jax.shard_map(
        functools.partial(on_device, mesh.shape["dp"], mesh.shape["tp"]),
        mesh=mesh,
        in_specs=in_specs,
        out_specs=out_specs,
        check_vma=False,
    )
```

```python
import functools

import jax
import jax.numpy as jnp
from jax import lax
from jax.experimental import pallas as pl
from jax.experimental.pallas import tpu as pltpu
from jax.sharding import PartitionSpec as P

NORM_EPS = 1e-06
MESH = pl.DeviceIdType.MESH
F32 = jnp.float32
BF16 = jnp.bfloat16
CHUNK_ROWS = 16
PIECES = 4
GELU_SLOPE = 0.7978845608028654

STAGE_AT = (0.0, 5.0, 9.5, 14.5, 19.5)
LAYER_AT = 22.0
CHUNK_AT = 4.0


def dot(a, b, contract=((1,), (0,)), precision=None):
    return lax.dot_general(
        a, b, (contract, ((), ())), preferred_element_type=F32, precision=precision
    )


def iota(shape, axis):
    return lax.broadcasted_iota(jnp.int32, shape, axis)


def expm1(x):
    p = jnp.full_like(x, 1.0 / 39916800.0)
    for d in (3628800.0, 362880.0, 40320.0, 5040.0, 720.0, 120.0, 24.0, 6.0, 2.0, 1.0):
        p = p * x + 1.0 / d
    return p * x


def column_of(row):
    n = row.shape[1]
    eye = iota((n, n), 0) == iota((n, n), 1)
    return jnp.sum(jnp.where(eye, row, 0.0), axis=1, keepdims=True)


def kernel(
    sizes,
    tok_ref,
    len_ref,
    state_ref,
    norm_ref,
    win_ref,
    wgate_ref,
    wout_ref,
    rate_ref,
    freq_ref,
    step_ref,
    gin_ref,
    gout_ref,
    feed_ref,
    decay_ref,
    out_tok,
    st,
    xs,
    seq,
    norm,
    win,
    wgate,
    wout,
    rate,
    freq,
    step,
    gin,
    gout,
    feed,
    decay,
    kb,
    rb,
    pay,
    got,
    zb,
    part,
    own,
    ab,
    load_sem,
    rs_send,
    rs_recv,
    ag_send,
    ag_recv,
    ar_send,
    ar_recv,
    x_send,
    x_recv,
):
    layers, dp, tp, chunks, rows, features = sizes
    groups, width = st.shape[2], st.shape[3]
    half = width // 2
    channels = win.shape[2]
    per_group = channels // groups
    blocks = groups // 8
    span = 8 * per_group
    total = features * dp
    pad = pay.shape[-1] - 2 * channels
    me = lax.axis_index("dp")
    z = lax.axis_index("tp")
    mid = tp // 2
    left = z < mid
    is_mid = jnp.logical_or(z == mid - 1, z == mid)
    is_end = jnp.logical_or(z == 0, z == tp - 1)
    inner = jnp.where(left, z + 1, z - 1)
    outer = jnp.where(left, z - 1, z + 1)
    peers = [lax.rem(me + k, dp) for k in range(1, dp)]

    loads = {}

    def load(name, src, dst):
        c = pltpu.make_async_copy(src, dst, load_sem.at[len(loads)])
        c.start()
        loads[name] = c

    load("x0", tok_ref.at[:, 0], xs.at[0, 0])
    load("norm", norm_ref, norm)
    load("win0", win_ref.at[0], win.at[0])
    load("wgate0", wgate_ref.at[0], wgate.at[0])
    for j in range(1, chunks):
        load(f"x{j}", tok_ref.at[:, j], xs.at[0, j])
    load("seq", len_ref, seq)
    load("rate", rate_ref, rate)
    load("freq", freq_ref, freq)
    load("step", step_ref, step)
    load("decay", decay_ref, decay)
    load("gin", gin_ref, gin)
    load("gout", gout_ref, gout)
    load("feed", feed_ref, feed)
    load("state0", state_ref.at[0], st.at[0])
    load("wout0", wout_ref.at[0], wout.at[0])
    for l in range(1, layers):
        load(f"state{l}", state_ref.at[l], st.at[l])
        load(f"win{l}", win_ref.at[l], win.at[l])
        load(f"wgate{l}", wgate_ref.at[l], wgate.at[l])
        load(f"wout{l}", wout_ref.at[l], wout.at[l])
    waited = set()

    def need(*names):
        for name in names:
            if name not in waited:
                waited.add(name)
                loads[name].wait()

    barrier = pltpu.get_barrier_semaphore()
    for p in peers:
        pl.semaphore_signal(barrier, inc=1, device_id={"dp": p}, device_id_type=MESH)
    pl.semaphore_signal(barrier, inc=1, device_id={"tp": inner}, device_id_type=MESH)

    @pl.when(jnp.logical_not(is_end))
    def _():
        pl.semaphore_signal(barrier, inc=1, device_id={"tp": outer}, device_id_type=MESH)

    pl.semaphore_wait(barrier, dp - 1 + jnp.where(is_end, 1, 2))

    def remote(src, dst, send, recv, axis, peer):
        return pltpu.make_async_remote_copy(
            src_ref=src,
            dst_ref=dst,
            send_sem=send,
            recv_sem=recv,
            device_id={axis: peer},
            device_id_type=MESH,
        )

    def rs_copy(l, j, k):
        return remote(
            pay.at[l, j, peers[k]], got.at[l, j, k], rs_send.at[l, j, k], rs_recv.at[l, j, k], "dp", peers[k]
        )

    def ag_copy(l, j, k):
        return remote(
            zb.at[l, j, me], zb.at[l, j, me], ag_send.at[l, j, k], ag_recv.at[l, j, k], "dp", peers[k]
        )

    def ag_arrival(l, j, k):
        origin = lax.rem(me + dp - (k + 1), dp)
        return remote(
            zb.at[l, j, me], zb.at[l, j, origin], ag_send.at[l, j, k], ag_recv.at[l, j, k], "dp", peers[k]
        )

    pieces = PIECES if dp % PIECES == 0 else 1
    cuts = [slice(p * dp // pieces, (p + 1) * dp // pieces) for p in range(pieces)]

    def sum_copy(l, j, p, slot=None):
        slot = jnp.where(is_mid, 1, 0) if slot is None else slot
        d = pl.ds(p * (dp // pieces), dp // pieces)
        return remote(
            own.at[l, j, d], ab.at[l, j, slot, d], ar_send.at[l, j, p], ar_recv.at[l, j, slot, p], "tp", inner
        )

    def x_copy(l, j, p):
        d = pl.ds(p * (dp // pieces), dp // pieces)
        there = after(l, j).at[d]
        return remote(there, there, x_send.at[l, j, p], x_recv.at[l, j, p], "tp", outer)

    def after(l, j):
        return xs.at[l + 1, j] if l + 1 < layers else out_tok.at[j]

    mask = (iota((1, 8, span), 2) // per_group) == iota((1, 8, span), 1)

    def prepare_tables():
        need("rate", "freq", "step", "gin", "gout")
        wide = groups * half
        pick = (iota((groups, wide), 1) // half) == iota((groups, wide), 0)
        sel = ((iota((wide, width), 0) % half) == (iota((wide, width), 1) % half)).astype(F32)
        sign = jnp.where(iota((1, width), 1) < half, 1.0, -1.0)
        tables = []
        for l in range(layers):
            both = jnp.concatenate(
                [jnp.where(pick, rate[l : l + 1], 0.0), jnp.where(pick, freq[l : l + 1], 0.0)], axis=0
            )
            flat = dot(both, sel, precision=lax.Precision.HIGHEST)
            a, w = flat[:groups], flat[groups:]
            dt = column_of(step[l : l + 1])
            log_mag = -a * dt
            turn = w * dt
            magnitude = jnp.exp(log_mag)
            cosine = jnp.cos(turn)
            dre = magnitude * cosine
            dim = magnitude * jnp.sin(turn)
            hs = jnp.sin(0.5 * turn)
            nre = expm1(log_mag) * cosine - 2.0 * hs * hs
            den = a * a + w * w
            kre = (-nre * a + dim * w) / den
            kim = (-dim * a - nre * w) / den
            b = gin[l]
            rolled = pltpu.roll(b.reshape(groups * per_group, width), half, 1).reshape(b.shape)
            kb[l] = (kre[:, None, :] * b - (sign * kim)[:, None, :] * rolled).astype(BF16).reshape(
                groups * per_group, width
            )
            rb[l] = (gout[l] * sign[None]).astype(BF16).reshape(groups * per_group, width)
            tables.append((dre, -sign * dim))
        return tables

    def prepare_state(l, tables, position):
        need(f"state{l}", "decay")
        dre, dim = tables[l]
        lg = decay[l]
        hi = lg.astype(BF16)
        lo = (lg - hi.astype(F32)).astype(BF16)
        e = jnp.exp(dot(position, hi, ((1,), (1,))) + dot(position, lo, ((1,), (1,))))
        seqs = e.shape[0]
        spread = jnp.broadcast_to(e[:, None, :], (seqs, 8, groups))
        for b in range(blocks):
            here = iota((1, 8, groups), 2) == (iota((1, 8, groups), 1) + 8 * b)
            factor = jnp.sum(jnp.where(here, spread, 0.0), axis=-1, keepdims=True)
            g = slice(8 * b, 8 * b + 8)
            s = st[l, :, g, :]
            turned = pltpu.roll(s.reshape(seqs * 8, width), half, 1).reshape(s.shape)
            st[l, :, g, :] = factor * (dre[g][None] * s + dim[g][None] * turned)

    def project(l, j):
        if l == 0:
            need(f"x{j}", "norm")
        need(f"win{l}", f"wgate{l}")
        x = xs[l, j].reshape(dp * rows, features).astype(F32)
        squares = jnp.sum(x * x, axis=1, keepdims=True)
        xg = (x * norm[l : l + 1]).astype(BF16)
        pay[l, j, :, :, :channels] = dot(xg, win[l]).astype(BF16).reshape(dp, rows, channels)
        pay[l, j, :, :, channels : 2 * channels] = dot(xg, wgate[l]).astype(BF16).reshape(dp, rows, channels)
        hi = squares.astype(BF16).astype(F32)
        lane = iota((dp * rows, pad), 1) < pad // 2
        pay[l, j, :, :, 2 * channels :] = (
            jnp.where(lane, hi, squares - hi).astype(BF16).reshape(dp, rows, pad)
        )
        for k in range(dp - 1):
            rs_copy(l, j, k).start()

    def update(l, j):
        for k in range(dp - 1):
            rs_copy(l, j, k).wait_recv()
        acc = pay[l, j, me].astype(F32)
        for k in range(dp - 1):
            acc = acc + got[l, j, k].astype(F32)
        squares = jnp.sum(acc[:, 2 * channels :], axis=1, keepdims=True) * (2.0 / pad)
        scale = lax.rsqrt(squares / total + NORM_EPS)
        u = (acc[:, :channels] * scale).astype(BF16).astype(F32)
        gate = (acc[:, channels : 2 * channels] * scale).astype(BF16).astype(F32)
        r = slice(j * rows, (j + 1) * rows)
        reads = []
        for b in range(blocks):
            ub = u[:, b * span : (b + 1) * span]
            spread = jnp.where(mask, jnp.broadcast_to(ub[:, None, :], (rows, 8, span)), 0.0)
            drive = dot(spread.reshape(rows * 8, span).astype(BF16), kb[l, b * span : (b + 1) * span])
            g = slice(8 * b, 8 * b + 8)
            new = st[l, r, g, :] + drive.reshape(rows, 8, width)
            st[l, r, g, :] = new
            read = dot(
                new.reshape(rows * 8, width).astype(BF16), rb[l, b * span : (b + 1) * span], ((1,), (1,))
            )
            reads.append(jnp.sum(jnp.where(mask, read.reshape(rows, 8, span), 0.0), axis=1))
        v = (jnp.concatenate(reads, axis=1) if blocks > 1 else reads[0]) + feed[l : l + 1] * u
        y = 0.5 * v * (1.0 + jnp.tanh(GELU_SLOPE * (v + 0.044715 * (v * v * v))))
        zb[l, j, me] = (y / (1.0 + jnp.exp(-gate))).astype(BF16)
        for k in range(dp - 1):
            ag_copy(l, j, k).start()

    def branch(l, j):
        need(f"wout{l}")
        for k in range(dp - 1):
            ag_arrival(l, j, k).wait_recv()
        term = dot(zb[l, j].reshape(dp * rows, channels), wout[l]).reshape(dp, rows, features)

        @pl.when(is_end)
        def _():
            for p, d in enumerate(cuts):
                own[l, j, d] = term[d].astype(BF16)
                sum_copy(l, j, p).start()

        @pl.when(jnp.logical_not(is_end))
        def _():
            part[l, j] = term

    def gather_in(l, j):
        @pl.when(jnp.logical_not(is_end))
        def _():
            for p, d in enumerate(cuts):
                sum_copy(l, j, p, 0).wait_recv()
                own[l, j, d] = (part[l, j, d] + ab[l, j, 0, d].astype(F32)).astype(BF16)
                sum_copy(l, j, p).start()

    def finish(l, j):
        @pl.when(is_mid)
        def _():
            for p, d in enumerate(cuts):
                sum_copy(l, j, p, 1).wait_recv()
                both = (own[l, j, d].astype(F32) + ab[l, j, 1, d].astype(F32)).astype(BF16)
                after(l, j)[d] = (xs[l, j, d].astype(F32) + both.astype(F32)).astype(BF16)

                @pl.when(jnp.logical_not(is_end))
                def _():
                    x_copy(l, j, p).start()

        @pl.when(jnp.logical_not(is_mid))
        def _():
            for p, d in enumerate(cuts):
                x_copy(l, j, p).wait_recv()

                @pl.when(jnp.logical_not(is_end))
                def _():
                    x_copy(l, j, p).start()

    stages = (project, update, branch, gather_in, finish)
    order = sorted(
        (l * LAYER_AT + STAGE_AT[s] + j * CHUNK_AT, l, s, j)
        for l in range(layers)
        for s in range(len(stages))
        for j in range(chunks)
    )
    tables = None
    for at, l, s, j in order:
        if s == 1 and tables is None:
            tables = prepare_tables()
            need("seq")
            lengths = column_of(seq[...].astype(F32)).astype(jnp.int32)
            places = decay.shape[2]
            position = (iota((lengths.shape[0], places), 1) == lengths - 1).astype(F32).astype(BF16)
            need("feed")
            for m in range(layers):
                prepare_state(m, tables, position)
        stages[s](l, j)

    for l in range(layers):
        for j in range(chunks):
            for k in range(dp - 1):
                rs_copy(l, j, k).wait_send()
                ag_copy(l, j, k).wait_send()
            for p in range(pieces):
                sum_copy(l, j, p).wait_send()

            @pl.when(jnp.logical_not(is_end))
            def _():
                for p in range(pieces):
                    x_copy(l, j, p).wait_send()


def on_device(
    dp,
    tp,
    tokens,
    sequence_lengths,
    recurrent_state,
    norm_weight,
    input_weight,
    gate_weight,
    output_weight,
    negated_real_rate,
    frequency,
    discrete_step,
    group_input_matrix,
    group_output_matrix,
    feedthrough_weight,
    extra_log_decay,
):
    batch, features = tokens.shape
    mine = sequence_lengths.shape[0]
    rows = CHUNK_ROWS if mine % CHUNK_ROWS == 0 else mine
    chunks = mine // rows
    layers = input_weight.shape[0]
    channels = input_weight.shape[2]
    pad = 128
    tall = 2 * channels + pad
    dma = pltpu.SemaphoreType.DMA
    any_spec = pl.BlockSpec(memory_space=pl.ANY)
    vmem = lambda a: pltpu.VMEM(a.shape, a.dtype)
    piece = (layers, chunks, dp, rows, features)
    n_tab = group_input_matrix.shape[1] * group_input_matrix.shape[2]
    width = group_input_matrix.shape[3]
    tok, state = pl.pallas_call(
        functools.partial(kernel, (layers, dp, tp, chunks, rows, features)),
        out_shape=(
            pltpu.VMEM((chunks, dp, rows, features), BF16),
            pltpu.VMEM(recurrent_state.shape, F32),
        ),
        in_specs=[any_spec] * 14,
        out_specs=(pl.BlockSpec(memory_space=pltpu.VMEM),) * 2,
        scratch_shapes=[
            pltpu.VMEM(piece, BF16),
            pltpu.VMEM((1, mine), jnp.int32),
            vmem(norm_weight),
            vmem(input_weight),
            vmem(gate_weight),
            vmem(output_weight),
            vmem(negated_real_rate),
            vmem(frequency),
            vmem(discrete_step),
            vmem(group_input_matrix),
            vmem(group_output_matrix),
            vmem(feedthrough_weight),
            vmem(extra_log_decay),
            pltpu.VMEM((layers, n_tab, width), BF16),
            pltpu.VMEM((layers, n_tab, width), BF16),
            pltpu.VMEM((layers, chunks, dp, rows, tall), BF16),
            pltpu.VMEM((layers, chunks, dp - 1, rows, tall), BF16),
            pltpu.VMEM((layers, chunks, dp, rows, channels), BF16),
            pltpu.VMEM(piece, F32),
            pltpu.VMEM(piece, BF16),
            pltpu.VMEM((layers, chunks, 2, dp, rows, features), BF16),
            dma((10 + chunks + 4 * layers,)),
            dma((layers, chunks, dp - 1)),
            dma((layers, chunks, dp - 1)),
            dma((layers, chunks, dp - 1)),
            dma((layers, chunks, dp - 1)),
            dma((layers, chunks, PIECES)),
            dma((layers, chunks, 2, PIECES)),
            dma((layers, chunks, PIECES)),
            dma((layers, chunks, PIECES)),
        ],
        compiler_params=pltpu.CompilerParams(
            collective_id=0, has_side_effects=True, vmem_limit_bytes=61 * 1024 * 1024
        ),
    )(
        tokens.reshape(dp, chunks, rows, features),
        sequence_lengths.reshape(1, mine),
        recurrent_state,
        norm_weight,
        input_weight,
        gate_weight,
        output_weight,
        negated_real_rate,
        frequency,
        discrete_step,
        group_input_matrix,
        group_output_matrix,
        feedthrough_weight,
        extra_log_decay,
    )
    return tok.transpose(1, 0, 2, 3).reshape(batch, features), state


def solution(mesh):
    in_specs = (
        P("grp", "dp"),
        P(("grp", "dp")),
        P(None, ("grp", "dp"), "tp", None),
        P(None, "dp"),
        P(None, "dp", "tp"),
        P(None, "dp", "tp"),
        P(None, "tp", "dp"),
        P(None, "tp"),
        P(None, "tp"),
        P(None, "tp"),
        P(None, "tp", None, None),
        P(None, "tp", None, None),
        P(None, "tp"),
        P(None, "tp", None),
    )
    out_specs = (P("grp", "dp"), P(None, ("grp", "dp"), "tp", None))
    return jax.shard_map(
        functools.partial(on_device, mesh.shape["dp"], mesh.shape["tp"]),
        mesh=mesh,
        in_specs=in_specs,
        out_specs=out_specs,
        check_vma=False,
    )
```
